32 devices in a mesh: sp: 8 (over z, x), tp: 4 (over y, core).
Axes of the slice: x: 2, y: 2, z: 4, core: 2. Of those that a mesh axis runs over, the one named last changes fastest.
Arguments:
- tokens: bfloat16 [6144, 4096], P('sp', 'tp'), may hold values from -6 to 6
- norm_gain: float32 [4096], replicated, may hold values from 0.1 to 1.9
- w_query: bfloat16 [4096, 2048], P('sp', 'tp'), may hold values from -0.09375 to 0.09375
- w_key: bfloat16 [4096, 1024], P('sp', 'tp'), may hold values from -0.09375 to 0.09375
- w_value: bfloat16 [4096, 1024], P('sp', 'tp'), may hold values from -0.09375 to 0.09375
- w_pool: bfloat16 [4096, 1024], P('sp', 'tp'), may hold values from -0.09375 to 0.09375
- query_gain: float32 [64], replicated, may hold values from 0.5 to 8
- key_gain: float32 [64], replicated, may hold values from 0.5 to 8
- sink_logit: float32 [32], P('tp'), may hold values from 1 to 5
- w_out_pool: bfloat16 [1024, 4096], P('tp', 'sp'), may hold values from -0.75 to 0.75
- w_out_attn: bfloat16 [2048, 4096], P('tp', 'sp'), may hold values from -1.5 to 1.5
Outputs:
- mixed: bfloat16 [6144, 4096], P(('sp', 'tp'))
The draws below stay inside these ranges and needn't reach their ends.
All inputs are finite; a program needn't handle non-finite values.
Results may differ from the reference program's by a relative error of at most 0.014.
The reference program's roundings to bfloat16 on the way count: a program that leaves them out, or rounds other values in their place, can miss the bound.
Values may be sent and summed in bfloat16 or wider, within the bound.
A program may use at most 128 MiB of HBM per device.

```python
import jax
import jax.numpy as jnp
from jax import lax

D = 4096
HEADS = 32
KV_HEADS = 16
HEAD = 64
POOL = 1024
WINDOW = 128
GRID_W = 64
SEQ = 6144
N_TP = 4


def draw_query_gain(key, part):
    return jax.random.uniform(jax.random.fold_in(key, 11), (HEAD,), jnp.float32, 0.5, 1.5)


def draw_key_gain(key, part):
    return jax.random.uniform(jax.random.fold_in(key, 23), (HEAD,), jnp.float32, 0.5, 1.5)


def shard_levels(key, extent, cuts, smallest, high):
    level = 1.0
    for dim, blocks in cuts:
        steps = jax.random.uniform(jax.random.fold_in(jax.random.fold_in(key, 6), dim), (blocks,), jnp.float32, smallest / len(cuts), high / len(cuts))
        level = level * jnp.repeat(jnp.exp(steps), extent[dim] // blocks).reshape((-1,) + (1,) * (len(extent) - 1 - dim))
    return level


def scatter_about(key, shape, spread, most, shards=(), kind=jnp.bfloat16):
    array = spread * jax.random.normal(key, shape, jnp.float32)
    if shards:
        array = array * shard_levels(key, shape, shards, -0.22, 0.18)
    return jnp.clip(array, -most, most).astype(kind)


def setup_inputs(seed: int = 0) -> dict:
    keys = jax.random.split(jax.random.key(seed), 12)
    return {
        "tokens": scatter_about(keys[0], (SEQ, D), 1.0, 6.0, ((0, 8), (1, 4))),
        "norm_gain": jnp.clip(1.0 + 0.18 * jax.random.normal(keys[1], (D,), jnp.float32), 0.1, 1.9),
        "w_query": scatter_about(keys[2], (D, HEADS * HEAD), D ** -0.5, 0.09375, ((0, 8), (1, 4))),
        "w_key": scatter_about(keys[3], (D, KV_HEADS * HEAD), D ** -0.5, 0.09375, ((0, 8), (1, 4))),
        "w_value": scatter_about(keys[4], (D, KV_HEADS * HEAD), D ** -0.5, 0.09375, ((0, 8), (1, 4))),
        "w_pool": scatter_about(keys[5], (D, POOL), D ** -0.5, 0.09375, ((0, 8), (1, 4))),
        "query_gain": draw_query_gain(jax.random.fold_in(keys[11], 71), 0),
        "key_gain": draw_key_gain(jax.random.fold_in(keys[11], 71), 0),
        "sink_logit": jnp.clip(1.0 + 4.0 * jax.random.uniform(keys[8], (HEADS,), jnp.float32) ** shard_levels(keys[8], (HEADS,), ((0, 4),), -0.2, 0.2), 1.0, 5.0),
        "w_out_pool": scatter_about(keys[9], (POOL, D), (POOL // 16) ** -0.5, 0.75, ((0, 4), (1, 8))),
        "w_out_attn": scatter_about(keys[10], (HEADS * HEAD, D), (HEADS * HEAD // 128) ** -0.5, 1.5, ((0, 4), (1, 8))),
    }


eps = 1e-06
rope_base = 10000.0
neg_big = -1e+30

def rope_tables(positions, head_size):
    quarter = head_size // 4
    freqs = 1.0 / rope_base ** (jnp.arange(quarter, dtype=jnp.float32) * 2.0 / (head_size // 2))
    row_angle = (positions // GRID_W).astype(jnp.float32)[:, None] * freqs
    col_angle = (positions % GRID_W).astype(jnp.float32)[:, None] * freqs
    angles = jnp.concatenate([row_angle, row_angle, col_angle, col_angle], axis=-1)
    return (jnp.cos(angles), jnp.sin(angles))

def rotate(heads_in, cosine, sine):
    part_one, part_two, part_three, part_four = jnp.split(heads_in, 4, axis=-1)
    turned = jnp.concatenate([-part_two, part_one, -part_four, part_three], axis=-1)
    return heads_in * cosine[:, None, :] + turned * sine[:, None, :]

def prepare(projected, gain, cosine, sine):
    rows_count = projected.shape[0]
    shaped = projected.reshape(rows_count, -1, HEAD)
    scaled = shaped * lax.rsqrt(lax.optimization_barrier(jnp.mean(shaped * shaped, axis=-1, keepdims=True)) + eps) * gain
    return rotate(scaled, cosine, sine).reshape(rows_count, -1).astype(jnp.bfloat16)

def reference(tokens, norm_gain, w_query, w_key, w_value, w_pool, query_gain, key_gain, sink_logit, w_out_pool, w_out_attn):
    seq = tokens.shape[0]
    widened = tokens.astype(jnp.float32)
    normed = (widened * lax.rsqrt(lax.optimization_barrier(jnp.mean(widened * widened, axis=1, keepdims=True)) + eps) * norm_gain).astype(jnp.bfloat16)
    query_raw = jnp.dot(normed, w_query, preferred_element_type=jnp.float32)
    key_raw = jnp.dot(normed, w_key, preferred_element_type=jnp.float32)
    values_all = jnp.dot(normed, w_value, preferred_element_type=jnp.float32).astype(jnp.bfloat16)
    pool_in = jnp.dot(normed, w_pool, preferred_element_type=jnp.float32).astype(jnp.bfloat16)
    positions = jnp.arange(seq, dtype=jnp.int32)
    cosine, sine = rope_tables(positions, HEAD)
    queries = prepare(query_raw, query_gain, cosine, sine)
    keys_all = prepare(key_raw, key_gain, cosine, sine)
    group = HEADS // KV_HEADS
    blocks = seq // WINDOW
    padded_keys = jnp.pad(keys_all, ((WINDOW, WINDOW), (0, 0)))
    padded_values = jnp.pad(values_all, ((WINDOW, WINDOW), (0, 0)))
    sink = sink_logit.astype(jnp.float32).reshape(KV_HEADS, group, 1, 1)

    def one_block(index):
        first_row = index * WINDOW
        block_q = lax.dynamic_slice_in_dim(queries, first_row, WINDOW, 0).reshape(WINDOW, KV_HEADS, group, HEAD).astype(jnp.float32)
        block_k = lax.dynamic_slice_in_dim(padded_keys, first_row, 3 * WINDOW, 0).reshape(3 * WINDOW, KV_HEADS, HEAD).astype(jnp.float32)
        block_v = lax.dynamic_slice_in_dim(padded_values, first_row, 3 * WINDOW, 0).reshape(3 * WINDOW, KV_HEADS, HEAD).astype(jnp.float32)
        scores = jnp.einsum('qhgd,khd->hgqk', block_q, block_k) * HEAD ** (-0.5)
        query_pos = first_row + jnp.arange(WINDOW, dtype=jnp.int32)[:, None]
        key_pos = first_row - WINDOW + jnp.arange(3 * WINDOW, dtype=jnp.int32)[None, :]
        inside = (jnp.abs(query_pos - key_pos) <= WINDOW) & (key_pos >= 0) & (key_pos < seq)
        scores = jnp.where(inside, scores, neg_big)
        top = jnp.maximum(lax.optimization_barrier(jnp.max(scores, axis=-1, keepdims=True)), sink)
        raised = jnp.exp(scores - top)
        totals = lax.optimization_barrier(jnp.sum(raised, axis=-1, keepdims=True)) + jnp.exp(sink - top)
        weights = (raised / totals).astype(jnp.bfloat16)
        result = jnp.einsum('hgqk,khd->qhgd', weights.astype(jnp.float32), block_v)
        return result.reshape(WINDOW, HEADS * HEAD).astype(jnp.bfloat16)
    attended = lax.map(one_block, jnp.arange(blocks, dtype=jnp.int32)).reshape(seq, HEADS * HEAD)
    pool_wide = pool_in.astype(jnp.float32)
    prefix = jnp.concatenate([jnp.zeros((1, POOL), jnp.float32), jnp.cumsum(pool_wide, axis=0)], axis=0)
    group_ch = POOL // 4
    levels = []
    for level in range(4):
        reach = 2 ** level
        low = jnp.clip(positions - reach, 0, seq - 1)
        high = jnp.clip(positions + reach - 1, 0, seq - 1)
        counted = (high - low + 1).astype(jnp.float32)
        columns = prefix[:, level * group_ch:(level + 1) * group_ch]
        summed = columns[high + 1] - columns[low]
        levels.append(summed / counted[:, None])
    pooled = jnp.concatenate(levels, axis=1).astype(jnp.bfloat16)
    pool_cols = POOL // N_TP
    attn_cols = HEADS * HEAD // N_TP
    outcome = jnp.zeros((seq, D), jnp.float32)
    for block_index in range(N_TP):
        term = jnp.dot(pooled[:, block_index * pool_cols:(block_index + 1) * pool_cols], w_out_pool[block_index * pool_cols:(block_index + 1) * pool_cols], preferred_element_type=jnp.float32)
        term = term + jnp.dot(attended[:, block_index * attn_cols:(block_index + 1) * attn_cols], w_out_attn[block_index * attn_cols:(block_index + 1) * attn_cols], preferred_element_type=jnp.float32)
        outcome = outcome + lax.optimization_barrier(term.astype(jnp.bfloat16)).astype(jnp.float32)
    return outcome.astype(jnp.bfloat16)
```

```python
import jax
import jax.numpy as jnp
from jax import lax
from jax.sharding import PartitionSpec as P

HEAD = 64
POOL = 1024
WINDOW = 128
GRID_W = 64


eps = 1e-06
rope_base = 10000.0
neg_big = -1e30
pool_reach = 8
longest_ring = 16


def padded_2(block, sides, width):
    for axis, dim in sides:
        count = lax.axis_size(axis)
        forward = [(i, i + 1) for i in range(count - 1)]
        backward = [(target, source) for source, target in forward]
        low = lax.ppermute(
            lax.slice_in_dim(block, block.shape[dim] - width, None, axis=dim), axis, forward
        )
        high = lax.ppermute(lax.slice_in_dim(block, 0, width, axis=dim), axis, backward)
        block = jnp.concatenate([low, block, high], axis=dim)
    return block


def rope_tables(positions, head_size):
    quarter = head_size // 4
    freqs = 1.0 / rope_base ** (jnp.arange(quarter, dtype=jnp.float32) * 2.0 / (head_size // 2))
    row_angle = (positions // GRID_W).astype(jnp.float32)[:, None] * freqs
    col_angle = (positions % GRID_W).astype(jnp.float32)[:, None] * freqs
    angles = jnp.concatenate([row_angle, row_angle, col_angle, col_angle], axis=-1)
    return (jnp.cos(angles), jnp.sin(angles))


def rotate(heads_in, cosine, sine):
    part_one, part_two, part_three, part_four = jnp.split(heads_in, 4, axis=-1)
    turned = jnp.concatenate([-part_two, part_one, -part_four, part_three], axis=-1)
    return heads_in * cosine[:, None, :] + turned * sine[:, None, :]


def prepare(projected, gain, cosine, sine):
    rows_count = projected.shape[0]
    shaped = projected.reshape(rows_count, -1, HEAD)
    scaled = shaped * lax.rsqrt(jnp.mean(shaped * shaped, axis=-1, keepdims=True) + eps) * gain
    return rotate(scaled, cosine, sine).reshape(rows_count, -1).astype(jnp.bfloat16)


def edge_keys(keys_new, values_new):
    joined = jnp.concatenate([keys_new, values_new], axis=1)
    return padded_2(joined, (("sp", 0),), WINDOW)


def edge_pool(pool_in):
    return padded_2(pool_in, (("sp", 0),), pool_reach)


def window_attention(queries, key_band, sink_logit, positions, seq):
    rows_count = queries.shape[0]
    key_width = key_band.shape[1] // 2
    heads_q = queries.shape[1] // HEAD
    heads_k = key_width // HEAD
    group = heads_q // heads_k
    blocks = rows_count // WINDOW
    stacked = key_band.reshape(blocks + 2, WINDOW, 2 * key_width)
    joined = jnp.concatenate([stacked[:-2], stacked[1:-1], stacked[2:]], axis=1)
    block_keys = joined[:, :, :key_width].reshape(blocks, 3 * WINDOW, heads_k, HEAD)
    block_values = joined[:, :, key_width:].reshape(blocks, 3 * WINDOW, heads_k, HEAD)
    block_queries = queries.reshape(blocks, WINDOW, heads_k, group, HEAD)
    scores = jnp.einsum(
        "nqhgd,nkhd->nhgqk", block_queries, block_keys, preferred_element_type=jnp.float32
    ) * HEAD ** (-0.5)
    query_pos = positions.reshape(blocks, WINDOW)
    key_pos = query_pos[:, :1] - WINDOW + jnp.arange(3 * WINDOW, dtype=jnp.int32)[None, :]
    inside = (
        (jnp.abs(query_pos[:, :, None] - key_pos[:, None, :]) <= WINDOW)
        & (key_pos[:, None, :] >= 0)
        & (key_pos[:, None, :] < seq)
    )
    scores = jnp.where(inside[:, None, None], scores, neg_big)
    sink = sink_logit.reshape(heads_k, group)[None, :, :, None, None]
    top = jnp.maximum(jnp.max(scores, axis=-1, keepdims=True), sink)
    raised = jnp.exp(scores - top)
    totals = jnp.sum(raised, axis=-1, keepdims=True) + jnp.exp(sink - top)
    weights = (raised / totals).astype(jnp.bfloat16)
    result = jnp.einsum(
        "nhgqk,nkhd->nqhgd", weights, block_values, preferred_element_type=jnp.float32
    )
    return result.astype(jnp.bfloat16).reshape(rows_count, heads_q * HEAD)


def window_pool(pool_band, pool_in, positions, seq):
    rows_count = pool_in.shape[0]
    level = lax.axis_index("tp") * pool_in.shape[1] // (POOL // 4)
    padded = pool_band.astype(jnp.float32)
    sum_two = padded[:-1] + padded[1:]
    sum_four = sum_two[:-2] + sum_two[2:]
    sum_eight = sum_four[:-4] + sum_four[4:]
    sum_sixteen = sum_eight[:-8] + sum_eight[8:]
    candidates = jnp.stack(
        [
            sum_two[7 : 7 + rows_count],
            sum_four[6 : 6 + rows_count],
            sum_eight[4 : 4 + rows_count],
            sum_sixteen[:rows_count],
        ]
    )
    chosen = lax.dynamic_index_in_dim(candidates, level, 0, keepdims=False)
    reach = jnp.left_shift(jnp.int32(1), level)
    low = jnp.clip(positions - reach, 0, seq - 1)
    high = jnp.clip(positions + reach - 1, 0, seq - 1)
    counted = (high - low + 1).astype(jnp.float32)
    return (chosen / counted[:, None]).astype(jnp.bfloat16)


def ring_order(count, across):
    deep = count // across
    if across == 1 or deep % 2:
        return list(range(count))
    order = [z * across for z in range(deep)]
    for turn, z in enumerate(reversed(range(deep))):
        row = range(1, across) if turn % 2 == 0 else reversed(range(1, across))
        order += [z * across + x for x in row]
    return order


def after(values, earlier):
    return lax.optimization_barrier((values, earlier))


def ring_gather(parts, order, axis):
    count = len(order)
    if count > longest_ring:
        ahead, _ = parts
        whole = tuple(lax.all_gather(part, "sp", axis=axis, tiled=True) for part in ahead)
        return [(None, whole)], (ahead, ahead)
    forward = [(order[i], order[(i + 1) % count]) for i in range(count)]
    backward = [(target, source) for source, target in forward]
    ahead, behind = parts
    arrived = [(0, ahead)]
    half = (count - 1) // 2
    for step in range(1, half + 1):
        ahead = tuple(lax.ppermute(part, "sp", forward) for part in ahead)
        behind = tuple(lax.ppermute(part, "sp", backward) for part in behind)
        arrived += [(-step, ahead), (step, behind)]
    last = (ahead, behind)
    if count % 2 == 0:
        opposite = (
            lax.ppermute(ahead[0], "sp", forward),
            lax.ppermute(behind[1], "sp", backward),
        )
        arrived.append((count // 2, opposite))
    return arrived, last


def gather_normed(tokens, norm_gain):
    rows, width = tokens.shape
    members = lax.axis_size("tp")
    chips = members // 2
    me = lax.axis_index("tp")
    chip, core = me // 2, me % 2
    pair = [(t, t ^ 1) for t in range(members)]
    blocks = [(me, tokens), (chip * 2 + 1 - core, lax.ppermute(tokens, "tp", pair))]
    for hop in range(1, chips):
        route = [
            (y * 2 + c, (y + hop) % chips * 2 + c) for y in range(chips) for c in range(2)
        ]
        far = lax.ppermute(tokens, "tp", route)
        source = (chip - hop + chips) % chips
        blocks.append((source * 2 + core, far))
        blocks.append((source * 2 + 1 - core, lax.ppermute(far, "tp", pair)))
    squares = 0.0
    for _, block in blocks:
        widened = block.astype(jnp.float32)
        squares = squares + jnp.sum(widened * widened, axis=1, keepdims=True)
    scale = lax.rsqrt(squares / (members * width) + eps)
    normed = jnp.zeros((rows, members * width), jnp.bfloat16)
    for owner, block in blocks:
        gain = lax.dynamic_slice_in_dim(norm_gain, owner * width, width, 0)
        piece = (block.astype(jnp.float32) * scale * gain).astype(jnp.bfloat16)
        normed = lax.dynamic_update_slice(normed, piece, (0, owner * width))
    return normed


def project(normed, arrived, order):
    count = len(order)
    place = jnp.array([order.index(i) for i in range(count)], jnp.int32)[lax.axis_index("sp")]
    owners = jnp.array(order, jnp.int32)
    totals = None
    for offset, parts in arrived:
        owner = 0 if offset is None else owners[(place + offset + count) % count]
        depth = parts[0].shape[0]
        columns = lax.dynamic_slice_in_dim(normed, owner * depth, depth, 1)
        terms = tuple(
            jnp.dot(columns, part, preferred_element_type=jnp.float32) for part in parts
        )
        totals = terms if totals is None else tuple(a + b for a, b in zip(totals, terms))
    return totals


def reduce_block(partial):
    rows, width = partial.shape
    members = lax.axis_size("tp")
    chips = members // 2
    me = lax.axis_index("tp")
    chip, core = me // 2, me % 2
    pair = [(t, t ^ 1) for t in range(members)]
    owned = partial.reshape(chips, 2, rows // members, width)
    away = lax.dynamic_index_in_dim(owned, 1 - core, 1, keepdims=False)
    kept = lax.dynamic_index_in_dim(owned, core, 1, keepdims=False)
    both = kept.astype(jnp.float32) + lax.ppermute(away, "tp", pair).astype(jnp.float32)
    total = lax.dynamic_index_in_dim(both, chip, 0, keepdims=False)
    for hop in range(1, chips):
        route = [
            (y * 2 + c, (y + hop) % chips * 2 + c) for y in range(chips) for c in range(2)
        ]
        out = lax.dynamic_index_in_dim(both, (chip + hop) % chips, 0, keepdims=False)
        total = total + lax.ppermute(out.astype(jnp.bfloat16), "tp", route).astype(jnp.float32)
    return total.astype(jnp.bfloat16)


def shards(
    tokens,
    norm_gain,
    w_query,
    w_key,
    w_value,
    w_pool,
    query_gain,
    key_gain,
    sink_logit,
    w_out_pool,
    w_out_attn,
):
    count = lax.axis_size("sp")
    order = ring_order(count, lax.axis_size("tp") // 2)
    rows_count = tokens.shape[0]
    positions = lax.axis_index("sp") * rows_count + jnp.arange(rows_count, dtype=jnp.int32)
    seq = count * rows_count
    cosine, sine = rope_tables(positions, HEAD)

    first = (jnp.concatenate([w_key, w_value], axis=1), w_pool)
    first_in, first_last = ring_gather((first, first), order, 0)
    middle = w_query.shape[1] // 2
    second = (w_query[:, :middle], w_query[:, middle:])
    second_ahead, _ = after(second, first_last[0])
    second_behind, _ = after(second, first_last[1])
    second_in, second_last = ring_gather((second_ahead, second_behind), order, 0)
    third = (w_out_pool, w_out_attn)
    third_ahead, _ = after(third, second_last[0])
    third_behind, _ = after(third, second_last[1])
    third_in, _ = ring_gather((third_ahead, third_behind), order, 1)

    normed = gather_normed(tokens, norm_gain)
    kv_raw, pool_raw = project(normed, first_in, order)
    key_width = w_key.shape[1]
    keys_new = prepare(kv_raw[:, :key_width], key_gain, cosine, sine)
    pool_in = pool_raw.astype(jnp.bfloat16)
    key_band = edge_keys(keys_new, kv_raw[:, key_width:].astype(jnp.bfloat16))
    pool_band = edge_pool(pool_in)
    pooled = window_pool(pool_band, pool_in, positions, seq)
    query_raw = jnp.concatenate(project(normed, second_in, order), axis=1)
    queries = prepare(query_raw, query_gain, cosine, sine)
    attended = window_attention(queries, key_band, sink_logit, positions, seq)

    place = jnp.array([order.index(i) for i in range(count)], jnp.int32)[lax.axis_index("sp")]
    owners = jnp.array(order, jnp.int32)
    width = w_out_pool.shape[1]
    mixed = jnp.zeros((rows_count // lax.axis_size("tp"), count * width), jnp.bfloat16)
    for offset, (out_pool, out_attn) in third_in:
        owner = 0 if offset is None else owners[(place + offset + count) % count]
        partial = (
            jnp.dot(pooled, out_pool, preferred_element_type=jnp.float32)
            + jnp.dot(attended, out_attn, preferred_element_type=jnp.float32)
        ).astype(jnp.bfloat16)
        mixed = lax.dynamic_update_slice(mixed, reduce_block(partial), (0, owner * width))
    return mixed


def solution(mesh):
    placed = (
        P("sp", "tp"),
        P(),
        P("sp", "tp"),
        P("sp", "tp"),
        P("sp", "tp"),
        P("sp", "tp"),
        P(),
        P(),
        P("tp"),
        P("tp", "sp"),
        P("tp", "sp"),
    )
    return jax.shard_map(
        shards, mesh=mesh, in_specs=placed, out_specs=P(("sp", "tp"), None), check_vma=False
    )
```

```python
import functools

import jax
import jax.numpy as jnp
from jax import lax
from jax.experimental import pallas as pl
from jax.experimental.pallas import tpu as pltpu
from jax.sharding import PartitionSpec as P

HEAD = 64
POOL = 1024
WINDOW = 128
GRID_W = 64


eps = 1e-06
rope_base = 10000.0
neg_big = -1e30
pool_reach = 8
longest_ring = 16


def padded_2(block, sides, width):
    for axis, dim in sides:
        count = lax.axis_size(axis)
        forward = [(i, i + 1) for i in range(count - 1)]
        backward = [(target, source) for source, target in forward]
        low = lax.ppermute(
            lax.slice_in_dim(block, block.shape[dim] - width, None, axis=dim), axis, forward
        )
        high = lax.ppermute(lax.slice_in_dim(block, 0, width, axis=dim), axis, backward)
        block = jnp.concatenate([low, block, high], axis=dim)
    return block


def rope_tables(positions, head_size):
    quarter = head_size // 4
    freqs = 1.0 / rope_base ** (jnp.arange(quarter, dtype=jnp.float32) * 2.0 / (head_size // 2))
    row_angle = (positions // GRID_W).astype(jnp.float32)[:, None] * freqs
    col_angle = (positions % GRID_W).astype(jnp.float32)[:, None] * freqs
    angles = jnp.concatenate([row_angle, row_angle, col_angle, col_angle], axis=-1)
    return (jnp.cos(angles), jnp.sin(angles))


def rotate(heads_in, cosine, sine):
    part_one, part_two, part_three, part_four = jnp.split(heads_in, 4, axis=-1)
    turned = jnp.concatenate([-part_two, part_one, -part_four, part_three], axis=-1)
    return heads_in * cosine[:, None, :] + turned * sine[:, None, :]


def prepare(projected, gain, cosine, sine):
    rows_count = projected.shape[0]
    shaped = projected.reshape(rows_count, -1, HEAD)
    scaled = shaped * lax.rsqrt(jnp.mean(shaped * shaped, axis=-1, keepdims=True) + eps) * gain
    return rotate(scaled, cosine, sine).reshape(rows_count, -1).astype(jnp.bfloat16)


def edge_keys(keys_new, values_new):
    joined = jnp.concatenate([keys_new, values_new], axis=1)
    return padded_2(joined, (("sp", 0),), WINDOW)


def edge_pool(pool_in):
    return padded_2(pool_in, (("sp", 0),), pool_reach)


def attention_kernel(seq, first_ref, sink_ref, raw_ref, gain_ref, cos_ref, sin_ref, band_ref, out_ref):
    step = pl.program_id(0)
    key_width = band_ref.shape[1] // 2
    heads_k = key_width // HEAD
    start = first_ref[0] + step * WINDOW
    lane = lax.broadcasted_iota(jnp.int32, (WINDOW, 2 * HEAD), 1)
    low_half = lane < HEAD
    lead = lane % (HEAD // 2) < HEAD // 4
    row = lax.broadcasted_iota(jnp.int32, (2 * WINDOW, 3 * WINDOW), 0) % WINDOW
    column = lax.broadcasted_iota(jnp.int32, (2 * WINDOW, 3 * WINDOW), 1)
    key_pos = start - WINDOW + column
    inside = (column >= row) & (column - row <= 2 * WINDOW) & (key_pos >= 0) & (key_pos < seq)
    top_row = lax.broadcasted_iota(jnp.int32, (2 * WINDOW, 1), 0) < WINDOW
    cosine, sine, gain = cos_ref[...], sin_ref[...], gain_ref[...]
    rows = pl.ds(pl.multiple_of(step * WINDOW, WINDOW), 3 * WINDOW)
    for head in range(heads_k):
        raw = raw_ref[:, head * 2 * HEAD : (head + 1) * 2 * HEAD]
        squares = raw * raw
        low_sum = jnp.sum(jnp.where(low_half, squares, 0.0), axis=1, keepdims=True)
        high_sum = jnp.sum(jnp.where(low_half, 0.0, squares), axis=1, keepdims=True)
        mean = jnp.where(low_half, low_sum, high_sum) * (1.0 / HEAD)
        scaled = raw * lax.rsqrt(mean + eps) * gain
        turned = jnp.where(
            lead,
            -pltpu.roll(scaled, 2 * HEAD - HEAD // 4, 1),
            pltpu.roll(scaled, HEAD // 4, 1),
        )
        query = (scaled * cosine + turned * sine) * HEAD ** (-0.5)
        other = pltpu.roll(query, HEAD, 1)
        if head % 2 == 0:
            pair = (jnp.where(low_half, query, 0.0), jnp.where(low_half, other, 0.0))
        else:
            pair = (jnp.where(low_half, 0.0, other), jnp.where(low_half, 0.0, query))
        stacked = jnp.concatenate(pair, axis=0).astype(jnp.bfloat16)
        tile = head // 2 * 2 * HEAD
        keys = band_ref[rows, tile : tile + 2 * HEAD]
        values = band_ref[rows, key_width + tile : key_width + tile + 2 * HEAD]
        scores = lax.dot_general(
            stacked, keys, (((1,), (1,)), ((), ())), preferred_element_type=jnp.float32
        )
        scores = jnp.where(inside, scores, neg_big)
        sink = jnp.where(top_row, sink_ref[2 * head], sink_ref[2 * head + 1])
        top = jnp.maximum(jnp.max(scores, axis=1, keepdims=True), sink)
        raised = jnp.exp(scores - top)
        totals = jnp.sum(raised, axis=1, keepdims=True) + jnp.exp(sink - top)
        weights = (raised * (1.0 / totals)).astype(jnp.bfloat16)
        result = jnp.dot(weights, values, preferred_element_type=jnp.float32)
        one, two = result[:WINDOW], result[WINDOW:]
        if head % 2 == 0:
            joined = jnp.where(low_half, one, pltpu.roll(two, HEAD, 1))
        else:
            joined = jnp.where(low_half, pltpu.roll(one, HEAD, 1), two)
        out_ref[:, head * 2 * HEAD : (head + 1) * 2 * HEAD] = joined.astype(jnp.bfloat16)


def window_attention(query_raw, query_gain, cosine, sine, key_band, sink_logit, first, seq):
    rows_count, width = query_raw.shape
    twice = lambda table: jnp.concatenate([table, table], axis=-1)
    by_row = lambda columns: pl.BlockSpec((WINDOW, columns), lambda i: (i, 0))
    in_smem = pl.BlockSpec(memory_space=pltpu.SMEM)
    return pl.pallas_call(
        functools.partial(attention_kernel, seq),
        grid=(rows_count // WINDOW,),
        out_shape=jax.ShapeDtypeStruct((rows_count, width), jnp.bfloat16),
        in_specs=[
            in_smem,
            in_smem,
            by_row(width),
            pl.BlockSpec((1, 2 * HEAD), lambda i: (0, 0)),
            by_row(2 * HEAD),
            by_row(2 * HEAD),
            pl.BlockSpec(key_band.shape, lambda i: (0, 0)),
        ],
        out_specs=by_row(width),
        cost_estimate=pl.CostEstimate(
            flops=12 * rows_count * width * 3 * WINDOW,
            bytes_accessed=16 * rows_count * width,
            transcendentals=rows_count * width // HEAD * 3 * WINDOW,
        ),
    )(
        first.reshape(1),
        sink_logit,
        query_raw,
        twice(query_gain).reshape(1, 2 * HEAD),
        twice(cosine),
        twice(sine),
        key_band,
    )


def window_pool(pool_band, pool_in, positions, seq):
    rows_count = pool_in.shape[0]
    level = lax.axis_index("tp") * pool_in.shape[1] // (POOL // 4)
    padded = pool_band.astype(jnp.float32)
    sum_two = padded[:-1] + padded[1:]
    sum_four = sum_two[:-2] + sum_two[2:]
    sum_eight = sum_four[:-4] + sum_four[4:]
    sum_sixteen = sum_eight[:-8] + sum_eight[8:]
    candidates = jnp.stack(
        [
            sum_two[7 : 7 + rows_count],
            sum_four[6 : 6 + rows_count],
            sum_eight[4 : 4 + rows_count],
            sum_sixteen[:rows_count],
        ]
    )
    chosen = lax.dynamic_index_in_dim(candidates, level, 0, keepdims=False)
    reach = jnp.left_shift(jnp.int32(1), level)
    low = jnp.clip(positions - reach, 0, seq - 1)
    high = jnp.clip(positions + reach - 1, 0, seq - 1)
    counted = (high - low + 1).astype(jnp.float32)
    return (chosen / counted[:, None]).astype(jnp.bfloat16)


def ring_order(count, across):
    deep = count // across
    if across == 1 or deep % 2:
        return list(range(count))
    order = [z * across for z in range(deep)]
    for turn, z in enumerate(reversed(range(deep))):
        row = range(1, across) if turn % 2 == 0 else reversed(range(1, across))
        order += [z * across + x for x in row]
    return order


def after(values, earlier):
    return lax.optimization_barrier((values, earlier))[0]


def ring_gather(parts, order, axis, gates=()):
    count = len(order)
    if count > longest_ring:
        ahead, _ = parts
        whole = tuple(lax.all_gather(part, "sp", axis=axis, tiled=True) for part in ahead)
        return [(None, whole)]
    forward = [(order[i], order[(i + 1) % count]) for i in range(count)]
    backward = [(target, source) for source, target in forward]
    ahead, behind = parts
    arrived = [(0, ahead)]
    half = (count - 1) // 2
    for step in range(1, half + 1):
        if step <= len(gates):
            ahead, behind = after(ahead, gates[step - 1][0]), after(behind, gates[step - 1][1])
        ahead = tuple(lax.ppermute(part, "sp", forward) for part in ahead)
        behind = tuple(lax.ppermute(part, "sp", backward) for part in behind)
        arrived += [(-step, ahead), (step, behind)]
    if half < len(gates):
        ahead, behind = after(ahead, gates[half][0]), after(behind, gates[half][1])
    if count % 2 == 0:
        opposite = (
            lax.ppermute(ahead[0], "sp", forward),
            lax.ppermute(behind[1], "sp", backward),
        )
        arrived.append((count // 2, opposite))
    return arrived


def gather_normed(tokens, norm_gain):
    rows, width = tokens.shape
    members = lax.axis_size("tp")
    chips = members // 2
    me = lax.axis_index("tp")
    chip, core = me // 2, me % 2
    pair = [(t, t ^ 1) for t in range(members)]
    blocks = [(me, tokens), (chip * 2 + 1 - core, lax.ppermute(tokens, "tp", pair))]
    for hop in range(1, chips):
        route = [
            (y * 2 + c, (y + hop) % chips * 2 + c) for y in range(chips) for c in range(2)
        ]
        far = lax.ppermute(tokens, "tp", route)
        source = (chip - hop + chips) % chips
        blocks.append((source * 2 + core, far))
        blocks.append((source * 2 + 1 - core, lax.ppermute(far, "tp", pair)))
    squares = 0.0
    for _, block in blocks:
        widened = block.astype(jnp.float32)
        squares = squares + jnp.sum(widened * widened, axis=1, keepdims=True)
    scale = lax.rsqrt(squares / (members * width) + eps)
    normed = jnp.zeros((rows, members * width), jnp.bfloat16)
    for owner, block in blocks:
        gain = lax.dynamic_slice_in_dim(norm_gain, owner * width, width, 0)
        piece = (block.astype(jnp.float32) * scale * gain).astype(jnp.bfloat16)
        normed = lax.dynamic_update_slice(normed, piece, (0, owner * width))
    return normed


def project(normed, arrived, order):
    count = len(order)
    place = jnp.array([order.index(i) for i in range(count)], jnp.int32)[lax.axis_index("sp")]
    owners = jnp.array(order, jnp.int32)
    totals = None
    steps = []
    for offset, parts in arrived:
        owner = 0 if offset is None else owners[(place + offset + count) % count]
        depth = parts[0].shape[0]
        columns = lax.dynamic_slice_in_dim(normed, owner * depth, depth, 1)
        terms = tuple(
            jnp.dot(columns, part, preferred_element_type=jnp.float32) for part in parts
        )
        totals = terms if totals is None else tuple(a + b for a, b in zip(totals, terms))
        steps.append(totals)
    return steps


def step_gates(arrived, steps):
    if len(arrived) < 8:
        return []
    last = len(steps) - 1
    whole = 2 * ((len(arrived) - 1) // 2)
    gates = [(arrived[whole - 1][1], arrived[whole][1])]
    for done in (2, whole, last):
        gates.append((steps[done], steps[done]))
    return gates


def reduce_block(partials):
    rows = partials[0].shape[0]
    members = lax.axis_size("tp")
    chips = members // 2
    me = lax.axis_index("tp")
    chip, core = me // 2, me % 2
    pair = [(t, t ^ 1) for t in range(members)]
    owned = [part.reshape(chips, 2, rows // members, -1) for part in partials]

    def rows_of(which):
        taken = [lax.dynamic_index_in_dim(part, which, 1, keepdims=False) for part in owned]
        return jnp.concatenate(taken, axis=2)

    away, kept = rows_of(1 - core), rows_of(core)
    both = kept.astype(jnp.float32) + lax.ppermute(away, "tp", pair).astype(jnp.float32)
    total = lax.dynamic_index_in_dim(both, chip, 0, keepdims=False)
    for hop in range(1, chips):
        route = [
            (y * 2 + c, (y + hop) % chips * 2 + c) for y in range(chips) for c in range(2)
        ]
        out = lax.dynamic_index_in_dim(both, (chip + hop) % chips, 0, keepdims=False)
        total = total + lax.ppermute(out.astype(jnp.bfloat16), "tp", route).astype(jnp.float32)
    return total.astype(jnp.bfloat16)


def shards(
    tokens,
    norm_gain,
    w_query,
    w_key,
    w_value,
    w_pool,
    query_gain,
    key_gain,
    sink_logit,
    w_out_pool,
    w_out_attn,
):
    count = lax.axis_size("sp")
    order = ring_order(count, lax.axis_size("tp") // 2)
    rows_count = tokens.shape[0]
    positions = lax.axis_index("sp") * rows_count + jnp.arange(rows_count, dtype=jnp.int32)
    seq = count * rows_count
    cosine, sine = rope_tables(positions, HEAD)

    normed = gather_normed(tokens, norm_gain)
    first = (jnp.concatenate([w_key, w_value], axis=1), w_pool)
    first_in = ring_gather((first, first), order, 0)
    first_steps = project(normed, first_in, order)
    kv_raw, pool_raw = first_steps[-1]
    key_width = w_key.shape[1]
    keys_new = prepare(kv_raw[:, :key_width], key_gain, cosine, sine)
    pool_in = pool_raw.astype(jnp.bfloat16)
    key_band = edge_keys(keys_new, kv_raw[:, key_width:].astype(jnp.bfloat16))
    pool_band = edge_pool(pool_in)
    pooled = window_pool(pool_band, pool_in, positions, seq)

    middle = w_query.shape[1] // 2
    second = (w_query[:, :middle], w_query[:, middle:])
    gates = step_gates(first_in, first_steps)
    second_in = ring_gather((second, second), order, 0, gates)
    second_steps = project(normed, second_in, order)
    query_raw = jnp.concatenate(second_steps[-1], axis=1)

    third = (w_out_pool, w_out_attn)
    gates = step_gates(second_in, second_steps)
    if gates:
        gates[1] = tuple((gate, key_band, pooled) for gate in gates[1])
    third_in = ring_gather((third, third), order, 1, gates)
    first_row = (lax.axis_index("sp") * rows_count).astype(jnp.int32)
    attended = window_attention(
        query_raw, query_gain, cosine, sine, key_band, sink_logit, first_row, seq
    )

    place = jnp.array([order.index(i) for i in range(count)], jnp.int32)[lax.axis_index("sp")]
    owners = jnp.array(order, jnp.int32)
    width = w_out_pool.shape[1]
    mixed = jnp.zeros((rows_count // lax.axis_size("tp"), count * width), jnp.bfloat16)
    groups = [third_in[:3]] + [third_in[i : i + 2] for i in range(3, len(third_in), 2)]
    for group in groups:
        partials = [
            (
                jnp.dot(pooled, out_pool, preferred_element_type=jnp.float32)
                + jnp.dot(attended, out_attn, preferred_element_type=jnp.float32)
            ).astype(jnp.bfloat16)
            for _, (out_pool, out_attn) in group
        ]
        reduced = reduce_block(partials)
        for index, (offset, _) in enumerate(group):
            owner = 0 if offset is None else owners[(place + offset + count) % count]
            piece = reduced if offset is None else reduced[:, index * width : (index + 1) * width]
            mixed = lax.dynamic_update_slice(mixed, piece, (0, owner * width))
    return mixed


def solution(mesh):
    placed = (
        P("sp", "tp"),
        P(),
        P("sp", "tp"),
        P("sp", "tp"),
        P("sp", "tp"),
        P("sp", "tp"),
        P(),
        P(),
        P("tp"),
        P("tp", "sp"),
        P("tp", "sp"),
    )
    return jax.shard_map(
        shards, mesh=mesh, in_specs=placed, out_specs=P(("sp", "tp"), None), check_vma=False
    )
```

```python
import functools

import jax
import jax.numpy as jnp
from jax import lax
from jax.experimental import pallas as pl
from jax.experimental.pallas import tpu as pltpu
from jax.sharding import PartitionSpec as P

HEAD = 64
POOL = 1024
WINDOW = 128
GRID_W = 64


eps = 1e-06
rope_base = 10000.0
neg_big = -1e30
pool_reach = 8
longest_ring = 16


def padded_2(block, sides, width):
    for axis, dim in sides:
        count = lax.axis_size(axis)
        forward = [(i, i + 1) for i in range(count - 1)]
        backward = [(target, source) for source, target in forward]
        low = lax.ppermute(
            lax.slice_in_dim(block, block.shape[dim] - width, None, axis=dim), axis, forward
        )
        high = lax.ppermute(lax.slice_in_dim(block, 0, width, axis=dim), axis, backward)
        block = jnp.concatenate([low, block, high], axis=dim)
    return block


def rope_tables(positions, head_size):
    quarter = head_size // 4
    freqs = 1.0 / rope_base ** (jnp.arange(quarter, dtype=jnp.float32) * 2.0 / (head_size // 2))
    row_angle = (positions // GRID_W).astype(jnp.float32)[:, None] * freqs
    col_angle = (positions % GRID_W).astype(jnp.float32)[:, None] * freqs
    angles = jnp.concatenate([row_angle, row_angle, col_angle, col_angle], axis=-1)
    return (jnp.cos(angles), jnp.sin(angles))


def rotate(heads_in, cosine, sine):
    part_one, part_two, part_three, part_four = jnp.split(heads_in, 4, axis=-1)
    turned = jnp.concatenate([-part_two, part_one, -part_four, part_three], axis=-1)
    return heads_in * cosine[:, None, :] + turned * sine[:, None, :]


def prepare(projected, gain, cosine, sine):
    rows_count = projected.shape[0]
    shaped = projected.reshape(rows_count, -1, HEAD)
    scaled = shaped * lax.rsqrt(jnp.mean(shaped * shaped, axis=-1, keepdims=True) + eps) * gain
    return rotate(scaled, cosine, sine).reshape(rows_count, -1).astype(jnp.bfloat16)


def edge_keys(keys_new, values_new):
    joined = jnp.concatenate([keys_new, values_new], axis=1)
    return padded_2(joined, (("sp", 0),), WINDOW)


def edge_pool(pool_in):
    return padded_2(pool_in, (("sp", 0),), pool_reach)


def attention_kernel(seq, first_ref, sink_ref, raw_ref, gain_ref, cos_ref, sin_ref, band_ref, out_ref):
    step = pl.program_id(0)
    key_width = band_ref.shape[1] // 2
    heads_k = key_width // HEAD
    start = first_ref[0] + step * WINDOW
    lane = lax.broadcasted_iota(jnp.int32, (WINDOW, 2 * HEAD), 1)
    low_half = lane < HEAD
    lead = lane % (HEAD // 2) < HEAD // 4
    row = lax.broadcasted_iota(jnp.int32, (2 * WINDOW, 3 * WINDOW), 0) % WINDOW
    column = lax.broadcasted_iota(jnp.int32, (2 * WINDOW, 3 * WINDOW), 1)
    key_pos = start - WINDOW + column
    inside = (column >= row) & (column - row <= 2 * WINDOW) & (key_pos >= 0) & (key_pos < seq)
    top_row = lax.broadcasted_iota(jnp.int32, (2 * WINDOW, 1), 0) < WINDOW
    cosine, sine, gain = cos_ref[...], sin_ref[...], gain_ref[...]
    rows = pl.ds(pl.multiple_of(step * WINDOW, WINDOW), 3 * WINDOW)
    for head in range(heads_k):
        raw = raw_ref[:, head * 2 * HEAD : (head + 1) * 2 * HEAD]
        squares = raw * raw
        low_sum = jnp.sum(jnp.where(low_half, squares, 0.0), axis=1, keepdims=True)
        high_sum = jnp.sum(jnp.where(low_half, 0.0, squares), axis=1, keepdims=True)
        mean = jnp.where(low_half, low_sum, high_sum) * (1.0 / HEAD)
        scaled = raw * lax.rsqrt(mean + eps) * gain
        turned = jnp.where(
            lead,
            -pltpu.roll(scaled, 2 * HEAD - HEAD // 4, 1),
            pltpu.roll(scaled, HEAD // 4, 1),
        )
        query = (scaled * cosine + turned * sine) * HEAD ** (-0.5)
        other = pltpu.roll(query, HEAD, 1)
        if head % 2 == 0:
            pair = (jnp.where(low_half, query, 0.0), jnp.where(low_half, other, 0.0))
        else:
            pair = (jnp.where(low_half, 0.0, other), jnp.where(low_half, 0.0, query))
        stacked = jnp.concatenate(pair, axis=0).astype(jnp.bfloat16)
        tile = head // 2 * 2 * HEAD
        keys = band_ref[rows, tile : tile + 2 * HEAD]
        values = band_ref[rows, key_width + tile : key_width + tile + 2 * HEAD]
        scores = lax.dot_general(
            stacked, keys, (((1,), (1,)), ((), ())), preferred_element_type=jnp.float32
        )
        scores = jnp.where(inside, scores, neg_big)
        sink = jnp.where(top_row, sink_ref[2 * head], sink_ref[2 * head + 1])
        top = jnp.maximum(jnp.max(scores, axis=1, keepdims=True), sink)
        raised = jnp.exp(scores - top)
        totals = jnp.sum(raised, axis=1, keepdims=True) + jnp.exp(sink - top)
        weights = (raised * (1.0 / totals)).astype(jnp.bfloat16)
        result = jnp.dot(weights, values, preferred_element_type=jnp.float32)
        one, two = result[:WINDOW], result[WINDOW:]
        if head % 2 == 0:
            joined = jnp.where(low_half, one, pltpu.roll(two, HEAD, 1))
        else:
            joined = jnp.where(low_half, pltpu.roll(one, HEAD, 1), two)
        out_ref[:, head * 2 * HEAD : (head + 1) * 2 * HEAD] = joined.astype(jnp.bfloat16)


def window_attention(query_raw, query_gain, cosine, sine, key_band, sink_logit, first, seq):
    rows_count, width = query_raw.shape
    twice = lambda table: jnp.concatenate([table, table], axis=-1)
    by_row = lambda columns: pl.BlockSpec((WINDOW, columns), lambda i: (i, 0))
    in_smem = pl.BlockSpec(memory_space=pltpu.SMEM)
    return pl.pallas_call(
        functools.partial(attention_kernel, seq),
        grid=(rows_count // WINDOW,),
        out_shape=jax.ShapeDtypeStruct((rows_count, width), jnp.bfloat16),
        in_specs=[
            in_smem,
            in_smem,
            by_row(width),
            pl.BlockSpec((1, 2 * HEAD), lambda i: (0, 0)),
            by_row(2 * HEAD),
            by_row(2 * HEAD),
            pl.BlockSpec(key_band.shape, lambda i: (0, 0)),
        ],
        out_specs=by_row(width),
        cost_estimate=pl.CostEstimate(
            flops=12 * rows_count * width * 3 * WINDOW,
            bytes_accessed=16 * rows_count * width,
            transcendentals=rows_count * width // HEAD * 3 * WINDOW,
        ),
    )(
        first.reshape(1),
        sink_logit,
        query_raw,
        twice(query_gain).reshape(1, 2 * HEAD),
        twice(cosine),
        twice(sine),
        key_band,
    )


def window_pool(pool_band, pool_in, positions, seq):
    rows_count = pool_in.shape[0]
    level = lax.axis_index("tp") * pool_in.shape[1] // (POOL // 4)
    padded = pool_band.astype(jnp.float32)
    sum_two = padded[:-1] + padded[1:]
    sum_four = sum_two[:-2] + sum_two[2:]
    sum_eight = sum_four[:-4] + sum_four[4:]
    sum_sixteen = sum_eight[:-8] + sum_eight[8:]
    candidates = jnp.stack(
        [
            sum_two[7 : 7 + rows_count],
            sum_four[6 : 6 + rows_count],
            sum_eight[4 : 4 + rows_count],
            sum_sixteen[:rows_count],
        ]
    )
    chosen = lax.dynamic_index_in_dim(candidates, level, 0, keepdims=False)
    reach = jnp.left_shift(jnp.int32(1), level)
    low = jnp.clip(positions - reach, 0, seq - 1)
    high = jnp.clip(positions + reach - 1, 0, seq - 1)
    counted = (high - low + 1).astype(jnp.float32)
    return (chosen / counted[:, None]).astype(jnp.bfloat16)


def ring_order(count, across):
    deep = count // across
    if across == 1 or deep % 2:
        return list(range(count))
    order = [z * across for z in range(deep)]
    for turn, z in enumerate(reversed(range(deep))):
        row = range(1, across) if turn % 2 == 0 else reversed(range(1, across))
        order += [z * across + x for x in row]
    return order


def after(values, earlier):
    return lax.optimization_barrier((values, earlier))[0]


def ring_gather(parts, order, axis, gate_of):
    count = len(order)
    if count > longest_ring:
        whole = tuple(lax.all_gather(part, "sp", axis=axis, tiled=True) for part in parts)
        return [(None, whole)]
    forward = [(order[i], order[(i + 1) % count]) for i in range(count)]
    backward = [(target, source) for source, target in forward]
    ahead = behind = parts
    arrived = [(0, parts)]
    half = (count - 1) // 2
    for step in range(1, half + 1):
        gate = gate_of(step, arrived)
        if gate is not None:
            ahead, behind = after(ahead, gate[0]), after(behind, gate[1])
        ahead = tuple(lax.ppermute(part, "sp", forward) for part in ahead)
        behind = tuple(lax.ppermute(part, "sp", backward) for part in behind)
        arrived += [(-step, ahead), (step, behind)]
    if count % 2 == 0:
        gate = gate_of(half + 1, arrived)
        if gate is not None:
            ahead, behind = after(ahead, gate[0]), after(behind, gate[1])
        opposite = (
            lax.ppermute(ahead[0], "sp", forward),
            lax.ppermute(behind[1], "sp", backward),
        )
        arrived.append((count // 2, opposite))
    return arrived


def gather_normed(tokens, norm_gain):
    rows, width = tokens.shape
    members = lax.axis_size("tp")
    chips = members // 2
    me = lax.axis_index("tp")
    chip, core = me // 2, me % 2
    pair = [(t, t ^ 1) for t in range(members)]
    blocks = [(me, tokens), (chip * 2 + 1 - core, lax.ppermute(tokens, "tp", pair))]
    for hop in range(1, chips):
        route = [
            (y * 2 + c, (y + hop) % chips * 2 + c) for y in range(chips) for c in range(2)
        ]
        far = lax.ppermute(tokens, "tp", route)
        source = (chip - hop + chips) % chips
        blocks.append((source * 2 + core, far))
        blocks.append((source * 2 + 1 - core, lax.ppermute(far, "tp", pair)))
    squares = 0.0
    for _, block in blocks:
        widened = block.astype(jnp.float32)
        squares = squares + jnp.sum(widened * widened, axis=1, keepdims=True)
    scale = lax.rsqrt(squares / (members * width) + eps)
    normed = jnp.zeros((rows, members * width), jnp.bfloat16)
    for owner, block in blocks:
        gain = lax.dynamic_slice_in_dim(norm_gain, owner * width, width, 0)
        piece = (block.astype(jnp.float32) * scale * gain).astype(jnp.bfloat16)
        normed = lax.dynamic_update_slice(normed, piece, (0, owner * width))
    return normed


def project(normed, arrived, order, steps):
    count = len(order)
    place = jnp.array([order.index(i) for i in range(count)], jnp.int32)[lax.axis_index("sp")]
    owners = jnp.array(order, jnp.int32)
    for offset, parts in arrived[len(steps) :]:
        owner = 0 if offset is None else owners[(place + offset + count) % count]
        depth = parts[0].shape[0]
        columns = lax.dynamic_slice_in_dim(normed, owner * depth, depth, 1)
        terms = tuple(
            jnp.dot(columns, part, preferred_element_type=jnp.float32) for part in parts
        )
        steps.append(tuple(a + b for a, b in zip(steps[-1], terms)) if steps else terms)


def reduce_block(partials):
    rows = partials[0].shape[0]
    members = lax.axis_size("tp")
    chips = members // 2
    me = lax.axis_index("tp")
    chip, core = me // 2, me % 2
    pair = [(t, t ^ 1) for t in range(members)]
    owned = [part.reshape(chips, 2, rows // members, -1) for part in partials]

    def rows_of(which):
        taken = [lax.dynamic_index_in_dim(part, which, 1, keepdims=False) for part in owned]
        return jnp.concatenate(taken, axis=2)

    away, kept = rows_of(1 - core), rows_of(core)
    met = lax.ppermute(away, "tp", pair)
    both = kept.astype(jnp.float32) + met.astype(jnp.float32)
    total = lax.dynamic_index_in_dim(both, chip, 0, keepdims=False)
    for hop in range(1, chips):
        route = [
            (y * 2 + c, (y + hop) % chips * 2 + c) for y in range(chips) for c in range(2)
        ]
        out = lax.dynamic_index_in_dim(both, (chip + hop) % chips, 0, keepdims=False)
        total = total + lax.ppermute(out.astype(jnp.bfloat16), "tp", route).astype(jnp.float32)
    return total.astype(jnp.bfloat16), met


def shards(
    tokens,
    norm_gain,
    w_query,
    w_key,
    w_value,
    w_pool,
    query_gain,
    key_gain,
    sink_logit,
    w_out_pool,
    w_out_attn,
):
    count = lax.axis_size("sp")
    order = ring_order(count, lax.axis_size("tp") // 2)
    rows_count = tokens.shape[0]
    positions = lax.axis_index("sp") * rows_count + jnp.arange(rows_count, dtype=jnp.int32)
    seq = count * rows_count
    cosine, sine = rope_tables(positions, HEAD)

    normed = gather_normed(tokens, norm_gain)
    steps = []

    def first_gate(step, arrived):
        if step < 3:
            return None
        project(normed, arrived[: 2 * step - 3], order, steps)
        return steps[-1], steps[-1]

    first = (jnp.concatenate([w_key, w_value, w_pool], axis=1), w_query)
    first_in = ring_gather(first, order, 0, first_gate)
    project(normed, first_in, order, steps)
    side_raw, query_raw = steps[-1]
    key_width, value_end = w_key.shape[1], w_key.shape[1] + w_value.shape[1]
    keys_new = prepare(side_raw[:, :key_width], key_gain, cosine, sine)
    pool_in = side_raw[:, value_end:].astype(jnp.bfloat16)
    key_band = edge_keys(keys_new, side_raw[:, key_width:value_end].astype(jnp.bfloat16))
    pool_band = edge_pool(pool_in)
    pooled = window_pool(pool_band, pool_in, positions, seq)

    def third_gate(step, arrived):
        whole = 2 * ((count - 1) // 2)
        if step == 1:
            ready = steps[max(whole - 2, 0)] if whole else steps[0]
            ends = (first_in[whole - 1][1], first_in[whole][1]) if whole else ((), ())
            return (ready, ends[0]), (ready, ends[1])
        if step == 2:
            return steps[whole], steps[whole]
        if step == 3:
            return steps[-1], steps[-1]
        return None

    third_in = ring_gather((w_out_pool, w_out_attn), order, 1, third_gate)
    query_raw = after(query_raw, tuple(parts for _, parts in third_in[3:5]))
    first_row = (lax.axis_index("sp") * rows_count).astype(jnp.int32)
    attended = window_attention(
        query_raw, query_gain, cosine, sine, key_band, sink_logit, first_row, seq
    )

    attended = after(attended, tuple(parts for _, parts in third_in[5:7]))

    place = jnp.array([order.index(i) for i in range(count)], jnp.int32)[lax.axis_index("sp")]
    owners = jnp.array(order, jnp.int32)
    width = w_out_pool.shape[1]
    mixed = jnp.zeros((rows_count // lax.axis_size("tp"), count * width), jnp.bfloat16)
    groups = [third_in[i : i + 2] for i in range(0, len(third_in), 2)]
    exchanged = []
    for group in groups:
        if len(exchanged) > 1:
            attended, pooled = after((attended, pooled), exchanged[-2])
        partials = [
            (
                jnp.dot(pooled, out_pool, preferred_element_type=jnp.float32)
                + jnp.dot(attended, out_attn, preferred_element_type=jnp.float32)
            ).astype(jnp.bfloat16)
            for _, (out_pool, out_attn) in group
        ]
        reduced, met = reduce_block(partials)
        exchanged.append(met)
        for index, (offset, _) in enumerate(group):
            owner = 0 if offset is None else owners[(place + offset + count) % count]
            piece = reduced if offset is None else reduced[:, index * width : (index + 1) * width]
            mixed = lax.dynamic_update_slice(mixed, piece, (0, owner * width))
    return mixed


def solution(mesh):
    placed = (
        P("sp", "tp"),
        P(),
        P("sp", "tp"),
        P("sp", "tp"),
        P("sp", "tp"),
        P("sp", "tp"),
        P(),
        P(),
        P("tp"),
        P("tp", "sp"),
        P("tp", "sp"),
    )
    return jax.shard_map(
        shards, mesh=mesh, in_specs=placed, out_specs=P(("sp", "tp"), None), check_vma=False
    )
```
